32 devices in a mesh: ep: 8 (over z, core), tp: 4 (over y, x).
Axes of the slice: x: 2, y: 2, z: 4, core: 2. Of those that a mesh axis runs over, the one named last changes fastest.
Arguments:
- tokens: bfloat16 [1536, 4096], P('ep'), may hold values from -6 to 6
- expert_ids: int32 [1536, 2], P('ep'), may hold values from 0 to 7, all different within a row; in each aligned block of 192 rows (0 to 191, 192 to 383, ...) at most 60 rows name the same one
- route_weight: float32 [1536, 2], P('ep'), may hold values from 0.1 to 1
- norm_gain: float32 [4096], replicated, may hold values from 0.1 to 1.9
- gate_weight: bfloat16 [8, 4096, 4096], P('ep', None, 'tp'), may hold values from -0.28125 to 0.28125
- up_weight: bfloat16 [8, 4096, 4096], P('ep', None, 'tp'), may hold values from -0.28125 to 0.28125
- down_weight: bfloat16 [8, 4096, 4096], P('ep', None, 'tp'), may hold values from -0.028076172 to 0.028076172
Outputs:
- mixed: bfloat16 [1536, 4096], P('ep', 'tp')
The draws below stay inside these ranges and needn't reach their ends.
Inputs may be any that keep to these rules, and one draw needn't show every extreme that they name: `expert_ids`: each row names 2 different experts. In each aligned block of 192 rows (the tokens of one index of ep) no expert is named by more than 60 rows, and in some block some expert is named by exactly 60 rows.
All inputs are finite; a program needn't handle non-finite values.
Results may differ from the reference program's by a relative error of at most 0.007.
Values may be sent and summed in bfloat16 or wider, within the bound.
A program may use at most 64 MiB of HBM per device.

```python
import math
import jax
import jax.numpy as jnp
import numpy as np
from jax import lax

D = 4096
FF = 4096
TOPK = 2
TOK_EP = 192
EXPERTS = 8
TOKENS = 1536
CAP = 60
N_EP = 8


def block_scale(key, extent, pieces, least, top_value):
    level, own = 1.0, jax.random.fold_in(key, 6)
    for axis_at, parts in pieces:
        draws = jnp.exp(jax.random.uniform(jax.random.fold_in(own, axis_at), (parts,), jnp.float32, least / len(pieces), top_value / len(pieces)))
        level = level * jnp.repeat(draws, extent[axis_at] // parts).reshape([-1 if axis == axis_at else 1 for axis in range(len(extent))])
    return level


def shared_out(stream_key, own, number, rows, number_of, top, bound, skew):
    ranking = jax.random.permutation(stream_key, number_of)
    heavy_load, usual = load_shares(number_of, rows * top, bound, skew, True), load_shares(number_of, rows * top, bound, skew, False)
    places = jnp.arange(number_of)

    def named(lengths, turn):
        used = int((lengths > 0).sum())
        fixed = max(1, used // 4)
        shifted = fixed + (places - fixed + turn * (used - fixed)) % max(1, number_of - fixed)
        return jnp.zeros((number_of,), jnp.int32).at[ranking[jnp.where(places < fixed, places, shifted)]].set(jnp.asarray(lengths, jnp.int32))

    lengths = jnp.where(number % 4 == 0, named(heavy_load, number // 4), named(usual, number - number // 4 - 1))
    mixed = jax.random.permutation(jax.random.fold_in(own, 3), number_of)
    source_of, receiver = mixed[0:number_of // 2 * 2:2], mixed[1:number_of // 2 * 2:2]
    margin = jnp.minimum(lengths[source_of] - 1, bound - lengths[receiver]) // 2
    margin = jnp.where((source_of == ranking[0]) | (receiver == ranking[0]) | (lengths[receiver] == 0), 0, jnp.maximum(margin, 0))
    shifted = jax.random.randint(jax.random.fold_in(own, 4), (number_of // 2,), 0, 1 << 20) % (margin + 1)
    lengths = lengths.at[source_of].add(-shifted).at[receiver].add(shifted)
    items = jnp.searchsorted(jnp.cumsum(lengths), jnp.arange(rows * top), side="right").astype(jnp.int32)
    listing = items.reshape(top, rows).T
    listing = listing[jax.random.permutation(jax.random.fold_in(own, 1), rows)]
    turn = jax.random.randint(jax.random.fold_in(own, 2), (rows, 1), 0, top)
    return jnp.take_along_axis(listing, (jnp.arange(top)[None, :] + turn) % top, axis=1)


def load_shares(count, total, bound, slope, full):
    weights = [(1 << 20) // math.isqrt(standing ** slope) + 1 for standing in range(1, count + 1)]
    largest = bound if full else min(bound, max(-(-total // count), total * weights[0] // sum(weights)))
    least = 1 if total - largest >= count - 1 else 0
    counts, rest = [largest] + [least] * (count - 1), total - largest - least * (count - 1)
    while rest > 0:
        candidates = [i for i in range(1, count) if counts[i] < largest] or [i for i in range(1, count) if counts[i] < bound]
        whole, left = sum([weights[i] for i in candidates]), rest
        for i in candidates:
            extra = min(bound - counts[i], max(1, left * weights[i] // whole), rest)
            counts[i] = counts[i] + extra
            rest = rest - extra
    return np.array(counts)


def scatter_about(stream_key, dims, deviation, bound, cuts=(), kind=jnp.bfloat16):
    gain = block_scale(stream_key, dims, cuts, -0.22, 0.18) if cuts else 1.0
    entries = jax.random.normal(stream_key, dims, jnp.float32) * deviation * gain
    return jnp.minimum(jnp.maximum(entries, -bound), bound).astype(kind)


def setup_inputs(seed: int = 0) -> dict:
    keys = jax.random.split(jax.random.key(seed), 8)
    tokens = scatter_about(keys[0], (TOKENS, D), 1.0, 6.0, ((0, 8),))
    expert_ids_keys = jax.random.split(jax.random.fold_in(keys[1], 1), TOKENS // TOK_EP)
    expert_ids_turns = jax.random.permutation(jax.random.fold_in(keys[1], 3), TOKENS // TOK_EP)
    expert_ids = jax.vmap(lambda own, number: shared_out(jax.random.fold_in(keys[1], 2), own, number, TOK_EP, EXPERTS, TOPK, CAP, 2))(expert_ids_keys, expert_ids_turns).reshape((TOKENS, TOPK))
    route_weight = jnp.clip(0.1 + 0.9 * jax.random.uniform(keys[2], (TOKENS, TOPK), jnp.float32) ** block_scale(keys[2], (TOKENS, TOPK), ((0, 8),), -0.2, 0.2), 0.1, 1.0)
    norm_gain = jnp.clip(1.0 + 0.18 * jax.random.normal(keys[3], (D,), jnp.float32), 0.1, 1.9)
    gate_weight = scatter_about(keys[4], (EXPERTS, D, FF), (3.0 / D ** 0.5), 0.28125, ((0, 8), (2, 4)))
    up_weight = scatter_about(keys[5], (EXPERTS, D, FF), (3.0 / D ** 0.5), 0.28125, ((0, 8), (2, 4)))
    down_weight = scatter_about(keys[6], (EXPERTS, FF, D), (0.3 / FF ** 0.5), 0.028076172, ((0, 8), (2, 4)))
    return {"tokens": tokens, "expert_ids": expert_ids, "route_weight": route_weight, "norm_gain": norm_gain, "gate_weight": gate_weight, "up_weight": up_weight, "down_weight": down_weight}


EPS = 1e-06
LIMIT = 7.0
ALPHA = 1.702

def rms_norm(tokens, norm_gain):
    values = tokens.astype(jnp.float32)
    scale = lax.rsqrt(lax.optimization_barrier(jnp.mean(values * values, axis=-1, keepdims=True)) + EPS)
    return (values * scale * norm_gain.astype(jnp.float32)).astype(jnp.bfloat16)

def clamped_unit(gate_pre, up_pre):
    gate = jnp.minimum(gate_pre, LIMIT)
    up_part = jnp.clip(up_pre, -LIMIT, LIMIT)
    return ((up_part + 1.0) * gate * jax.nn.sigmoid(ALPHA * gate)).astype(jnp.bfloat16)

def reference(tokens, expert_ids, route_weight, norm_gain, gate_weight, up_weight, down_weight):
    normed = rms_norm(tokens, norm_gain)
    copies = TOK_EP * TOPK
    ids_blocks = expert_ids.reshape(N_EP, copies).astype(jnp.int32)
    onehot = (ids_blocks[:, :, None] == jnp.arange(EXPERTS, dtype=jnp.int32)[None, None, :]).astype(jnp.int32)
    before = jnp.cumsum(onehot, axis=1) - onehot
    position = lax.optimization_barrier(jnp.sum(before * onehot, axis=2)).astype(jnp.int32)
    block_ids = jnp.broadcast_to(jnp.arange(N_EP, dtype=jnp.int32)[:, None], (N_EP, copies))
    copy_token = (block_ids * TOK_EP + jnp.arange(copies, dtype=jnp.int32)[None, :] // TOPK).astype(jnp.int32)
    table = jnp.full((EXPERTS, N_EP, CAP), TOKENS, jnp.int32)
    table = table.at[ids_blocks, block_ids, position].set(copy_token)
    weight_table = jnp.zeros((EXPERTS, N_EP, CAP), jnp.float32)
    weight_table = weight_table.at[ids_blocks, block_ids, position].set(route_weight.reshape(N_EP, copies).astype(jnp.float32))
    padded = jnp.concatenate([normed, jnp.zeros((1, D), jnp.bfloat16)], axis=0)

    def one_expert(operands):
        gate_w, up_w, down_w, row_index, weights = operands
        rows = padded[row_index.reshape(-1)]
        gate_pre = jnp.dot(rows, gate_w, preferred_element_type=jnp.float32)
        up_pre = jnp.dot(rows, up_w, preferred_element_type=jnp.float32)
        hidden = clamped_unit(gate_pre, up_pre)
        result = jnp.dot(hidden, down_w, preferred_element_type=jnp.float32).astype(jnp.bfloat16)
        result = lax.optimization_barrier(result).astype(jnp.float32)
        return result * weights.reshape(-1)[:, None]
    outputs = lax.map(one_expert, (gate_weight, up_weight, down_weight, table, weight_table))
    total = jnp.zeros((TOKENS + 1, D), jnp.float32)
    total = total.at[table.reshape(-1)].add(outputs.reshape(-1, D))
    return total[:TOKENS].astype(jnp.bfloat16)
```

```python
import functools

import jax
import jax.numpy as jnp
from jax import lax
from jax.experimental import pallas as pl
from jax.experimental.pallas import tpu as pltpu
from jax.sharding import PartitionSpec as P

EPS = 1e-06
LIMIT = 7.0
ALPHA = 1.702


def rms_norm(tokens, norm_gain):
    values = tokens.astype(jnp.float32)
    scale = lax.rsqrt(jnp.mean(values * values, axis=-1, keepdims=True) + EPS)
    return (values * scale * norm_gain).astype(jnp.bfloat16)


def clamped_unit(gate_pre, up_pre):
    gate = jnp.minimum(gate_pre, LIMIT)
    up_part = jnp.clip(up_pre, -LIMIT, LIMIT)
    return ((up_part + 1.0) * gate * jax.nn.sigmoid(ALPHA * gate)).astype(jnp.bfloat16)


def slot_numbers(id_blocks, experts, capacity):
    onehot = (id_blocks[:, :, None] == jnp.arange(experts, dtype=jnp.int32)[None, None, :]).astype(
        jnp.int32
    )
    before = jnp.cumsum(onehot, axis=1) - onehot
    position = jnp.sum(before * onehot, axis=2)
    return id_blocks * capacity + position


def project_down(hidden, down_weight):
    result = jnp.einsum(
        "sejf,efd->sejd",
        lax.all_gather(hidden, "tp", axis=3, tiled=True),
        down_weight,
        preferred_element_type=jnp.float32,
    )
    return result.astype(jnp.bfloat16)


def plain_path(tokens, expert_ids, route_weight, norm_gain, gate_weight, up_weight, down_weight):
    n_ep = lax.axis_size("ep")
    n_tp = lax.axis_size("tp")
    tok_rows, width = tokens.shape
    top = expert_ids.shape[1]
    local_experts = gate_weight.shape[0]
    experts = local_experts * n_ep
    capacity = 5 * tok_rows * top // (4 * experts)
    cols = width // n_tp
    normed = rms_norm(tokens, norm_gain)
    dest = slot_numbers(expert_ids.reshape(1, tok_rows * top), experts, capacity).reshape(-1)
    slot_range = jnp.arange(experts * capacity, dtype=jnp.int32)
    match = slot_range[:, None] == dest[None, :]
    pick = jnp.any(match.reshape(experts * capacity, tok_rows, top), axis=2).astype(jnp.bfloat16)
    own = lax.dynamic_slice_in_dim(normed, lax.axis_index("tp") * cols, cols, 1)
    buffer = jnp.dot(pick, own, preferred_element_type=jnp.float32).astype(jnp.bfloat16)
    buffer = buffer.reshape(n_ep, local_experts, capacity, cols)
    arrived = lax.all_to_all(buffer, "ep", split_axis=0, concat_axis=0, tiled=True)
    piece = lax.all_gather(arrived, "tp", axis=3, tiled=True)
    gate_part = jnp.einsum("sejd,edf->sejf", piece, gate_weight, preferred_element_type=jnp.float32)
    up_part = jnp.einsum("sejd,edf->sejf", piece, up_weight, preferred_element_type=jnp.float32)
    hidden = clamped_unit(gate_part, up_part)
    result = project_down(hidden, down_weight)
    back = lax.all_to_all(result, "ep", split_axis=0, concat_axis=0, tiled=True).reshape(
        experts * capacity, cols
    )
    chosen = jnp.transpose(match).astype(jnp.bfloat16)
    per_copy = jnp.dot(chosen, back, preferred_element_type=jnp.float32).reshape(
        tok_rows, top, cols
    )
    mixed = jnp.sum(per_copy * route_weight[:, :, None], axis=1)
    return mixed.astype(jnp.bfloat16)


VMEM_BYTES = 60 * 1024 * 1024
COLUMN_TILE = 256


def flip(value, bits):
    bit = 1
    while bit <= bits:
        if bits & bit:
            value = value + bit - 2 * bit * lax.rem(lax.div(value, jnp.int32(bit)), jnp.int32(2))
        bit *= 2
    return value


def fused_kernel(
    n_ep,
    n_tp,
    slots,
    tokens_ref,
    ids_ref,
    ids_row_ref,
    route_ref,
    gain_ref,
    gate_hbm,
    up_hbm,
    down_hbm,
    out_ref,
    gate_v,
    up_v,
    down_v,
    normed,
    outbox,
    fullbox,
    xbuf,
    hbuf,
    obuf,
    back,
    weight_sem,
    z_send,
    z_recv,
    pair_send,
    pair_recv,
    g_send,
    g_recv,
    b_send,
    b_recv,
):
    pairs = n_ep // 2
    tok_rows = tokens_ref.shape[0]
    cols = xbuf.shape[-1]
    hid = hbuf.shape[-1]
    outs = obuf.shape[-1]
    ep = lax.axis_index("ep")
    tp = lax.axis_index("tp")
    pair = lax.div(ep, jnp.int32(2))
    core = lax.rem(ep, jnp.int32(2))
    side = (flip(tp, 1), flip(tp, 2))
    far = flip(tp, 3)

    loads = [
        pltpu.make_async_copy(hbm.at[0], vmem, weight_sem.at[i])
        for i, (hbm, vmem) in enumerate(((gate_hbm, gate_v), (up_hbm, up_v), (down_hbm, down_v)))
    ]
    for load in loads:
        load.start()

    barrier = pltpu.get_barrier_semaphore()
    for k in range(1, n_ep):
        pl.semaphore_signal(
            barrier, inc=1, device_id=(flip(ep, k), tp), device_id_type=pl.DeviceIdType.MESH
        )
    for other in side:
        pl.semaphore_signal(
            barrier, inc=1, device_id=(ep, other), device_id_type=pl.DeviceIdType.MESH
        )

    def norm_rows(i, carry):
        rows = pl.ds(pl.multiple_of(i * 16, 16), 16)
        values = tokens_ref[rows, :].astype(jnp.float32)
        scale = lax.rsqrt(jnp.mean(values * values, axis=-1, keepdims=True) + EPS)
        normed[rows, :] = (values * scale * gain_ref[...]).astype(jnp.bfloat16)
        return carry

    lax.fori_loop(0, tok_rows // 16, norm_rows, 0)

    ids_row = ids_row_ref[...]
    expert_col = lax.broadcasted_iota(jnp.int32, (n_ep, tok_rows), 0)
    hits_row = ((ids_row[0:1, :] == expert_col) | (ids_row[1:2, :] == expert_col)).astype(
        jnp.float32
    ).astype(jnp.bfloat16)
    first = lax.broadcasted_iota(jnp.int32, (tok_rows, tok_rows), 0)
    second = lax.broadcasted_iota(jnp.int32, (tok_rows, tok_rows), 1)
    earlier = (first < second).astype(jnp.float32).astype(jnp.bfloat16)
    before_row = jnp.dot(hits_row, earlier, preferred_element_type=jnp.float32)
    slot_row = [
        jnp.sum(jnp.where(ids_row[k : k + 1, :] == expert_col, before_row, 0.0), axis=0, keepdims=True)
        for k in range(2)
    ]
    slot_at = lax.broadcasted_iota(jnp.int32, (slots, tok_rows), 0).astype(jnp.float32)

    def pick_of(expert):
        taken = ((ids_row[0:1, :] == expert) & (slot_row[0] == slot_at)) | (
            (ids_row[1:2, :] == expert) & (slot_row[1] == slot_at)
        )
        return taken.astype(jnp.float32).astype(jnp.bfloat16)

    pl.semaphore_wait(barrier, n_ep - 1 + 2)

    own_cols = pl.ds(pl.multiple_of(tp * cols, cols), cols)

    def z_copy(k, c):
        return pltpu.make_async_remote_copy(
            src_ref=outbox.at[k - 1, c],
            dst_ref=xbuf.at[k, tp, core],
            send_sem=z_send.at[k, c],
            recv_sem=z_recv.at[k, core],
            device_id=(flip(pair, k) * 2 + c, tp),
            device_id_type=pl.DeviceIdType.MESH,
        )

    def z_arrival(k, c):
        return pltpu.make_async_remote_copy(
            src_ref=outbox.at[k - 1, c],
            dst_ref=xbuf.at[k, tp, c],
            send_sem=z_send.at[k, c],
            recv_sem=z_recv.at[k, c],
            device_id=(flip(pair, k) * 2 + c, tp),
            device_id_type=pl.DeviceIdType.MESH,
        )

    for k in range(1, pairs):
        for c in range(2):
            outbox[k - 1, c] = jnp.dot(
                pick_of(flip(pair, k) * 2 + c),
                normed[:, own_cols],
                preferred_element_type=jnp.float32,
            ).astype(jnp.bfloat16)
            z_copy(k, c).start()

    partner = flip(ep, 1)
    pair_copy = pltpu.make_async_remote_copy(
        src_ref=fullbox,
        dst_ref=xbuf.at[0, :, core],
        send_sem=pair_send,
        recv_sem=pair_recv,
        device_id=(partner, tp),
        device_id_type=pl.DeviceIdType.MESH,
    )
    pair_arrival = pltpu.make_async_remote_copy(
        src_ref=fullbox,
        dst_ref=xbuf.at[0, :, 1 - core],
        send_sem=pair_send,
        recv_sem=pair_recv,
        device_id=(partner, tp),
        device_id_type=pl.DeviceIdType.MESH,
    )
    theirs = pick_of(partner)
    for j in range(n_tp):
        fullbox[j] = jnp.dot(
            theirs, normed[:, j * cols : (j + 1) * cols], preferred_element_type=jnp.float32
        ).astype(jnp.bfloat16)
    pair_copy.start()
    mine = pick_of(ep)
    for j in range(n_tp):
        xbuf[0, j, core] = jnp.dot(
            mine, normed[:, j * cols : (j + 1) * cols], preferred_element_type=jnp.float32
        ).astype(jnp.bfloat16)

    boxes = (xbuf, hbuf)

    def block_copy(b, k, d, half):
        return pltpu.make_async_remote_copy(
            src_ref=boxes[b].at[k, tp, half],
            dst_ref=boxes[b].at[k, tp, half],
            send_sem=g_send.at[b, k, 2 * d + half],
            recv_sem=g_recv.at[b, k, 2 * d + half],
            device_id=(ep, side[d]),
            device_id_type=pl.DeviceIdType.MESH,
        )

    def block_arrival(b, k, d, half):
        return pltpu.make_async_remote_copy(
            src_ref=boxes[b].at[k, side[d], half],
            dst_ref=boxes[b].at[k, side[d], half],
            send_sem=g_send.at[b, k, 2 * d + half],
            recv_sem=g_recv.at[b, k, 2 * d + half],
            device_id=(ep, side[d]),
            device_id_type=pl.DeviceIdType.MESH,
        )

    def relay_copy(b, k, d):
        return pltpu.make_async_remote_copy(
            src_ref=boxes[b].at[k, side[d], d],
            dst_ref=boxes[b].at[k, side[d], d],
            send_sem=g_send.at[b, k, 4 + d],
            recv_sem=g_recv.at[b, k, 4 + d],
            device_id=(ep, side[1 - d]),
            device_id_type=pl.DeviceIdType.MESH,
        )

    def relay_arrival(b, k, d):
        return pltpu.make_async_remote_copy(
            src_ref=boxes[b].at[k, far, d],
            dst_ref=boxes[b].at[k, far, d],
            send_sem=g_send.at[b, k, 4 + d],
            recv_sem=g_recv.at[b, k, 4 + d],
            device_id=(ep, side[1 - d]),
            device_id_type=pl.DeviceIdType.MESH,
        )

    def spread(b, k):
        for step in range(2):
            for d in range(2):
                block_copy(b, k, d, d if step == 0 else 1 - d).start()

    def relay(b, k):
        for d in range(2):
            block_arrival(b, k, d, d).wait_recv()
            relay_copy(b, k, d).start()

    def gathered(b, k):
        for d in range(2):
            block_arrival(b, k, d, 1 - d).wait_recv()
        for d in range(2):
            relay_arrival(b, k, d).wait_recv()

    def enter(k):
        for c in range(2):
            z_arrival(k, c).wait_recv()
        spread(0, k)

    def dot_blocks(box, k, weight, where):
        depth = box.shape[-1]
        total = None
        for j in range(n_tp):
            part = jnp.dot(
                box[k, j].reshape(2 * slots, depth),
                weight[j * depth : (j + 1) * depth, where],
                preferred_element_type=jnp.float32,
            )
            total = part if total is None else total + part
        return total

    def units(k):
        def tile(i, carry):
            where = pl.ds(pl.multiple_of(i * COLUMN_TILE, COLUMN_TILE), COLUMN_TILE)
            gate_pre = dot_blocks(xbuf, k, gate_v, where)
            up_pre = dot_blocks(xbuf, k, up_v, where)
            hidden = clamped_unit(gate_pre, up_pre)
            hbuf[k, tp, :, :, where] = hidden.reshape(2, slots, COLUMN_TILE)
            return carry

        lax.fori_loop(0, hid // COLUMN_TILE, tile, 0)
        spread(1, k)

    def back_copy(k, c):
        return pltpu.make_async_remote_copy(
            src_ref=obuf.at[k, c],
            dst_ref=back.at[ep],
            send_sem=b_send.at[k, c],
            recv_sem=b_recv.at[ep],
            device_id=(flip(pair, k) * 2 + c, tp),
            device_id_type=pl.DeviceIdType.MESH,
        )

    def back_arrival(flips):
        other = flip(ep, flips)
        return pltpu.make_async_remote_copy(
            src_ref=obuf.at[0, 0],
            dst_ref=back.at[other],
            send_sem=b_send.at[0, 0],
            recv_sem=b_recv.at[other],
            device_id=(other, tp),
            device_id_type=pl.DeviceIdType.MESH,
        )

    partner_back = pltpu.make_async_remote_copy(
        src_ref=obuf.at[0, 1 - core],
        dst_ref=back.at[ep],
        send_sem=b_send.at[0, 0],
        recv_sem=b_recv.at[ep],
        device_id=(partner, tp),
        device_id_type=pl.DeviceIdType.MESH,
    )

    def results(k):
        def tile(i, carry):
            where = pl.ds(pl.multiple_of(i * COLUMN_TILE, COLUMN_TILE), COLUMN_TILE)
            total = dot_blocks(hbuf, k, down_v, where).astype(jnp.bfloat16)
            obuf[k, :, :, where] = total.reshape(2, slots, COLUMN_TILE)
            return carry

        lax.fori_loop(0, outs // COLUMN_TILE, tile, 0)
        if k == 0:
            partner_back.start()
            back[ep] = obuf[0, core]
        else:
            for c in range(2):
                back_copy(k, c).start()

    loads[0].wait()
    loads[1].wait()
    pair_arrival.wait_recv()
    units(0)
    enter(1)
    relay(1, 0)
    if pairs > 2:
        enter(2)
    relay(0, 1)
    loads[2].wait()
    gathered(1, 0)
    results(0)
    for k in range(1, pairs):
        gathered(0, k)
        units(k)
        if k + 2 < pairs:
            enter(k + 2)
        if k + 1 < pairs:
            relay(0, k + 1)
            relay(1, k)
        if k >= 2:
            gathered(1, k - 1)
            results(k - 1)
    relay(1, pairs - 1)
    gathered(1, pairs - 1)
    results(pairs - 1)

    expert_row = lax.broadcasted_iota(jnp.int32, (tok_rows, n_ep), 1)
    ids = [ids_ref[:, k : k + 1] for k in range(2)]
    hits = ((ids[0] == expert_row) | (ids[1] == expert_row)).astype(jnp.float32).astype(jnp.bfloat16)
    later = (second < first).astype(jnp.float32).astype(jnp.bfloat16)
    before = jnp.dot(later, hits, preferred_element_type=jnp.float32)
    place = lax.broadcasted_iota(jnp.int32, (tok_rows, n_ep * slots), 1).astype(jnp.float32)
    chosen = []
    for k in range(2):
        slot = jnp.sum(jnp.where(ids[k] == expert_row, before, 0.0), axis=1, keepdims=True)
        spot = ids[k].astype(jnp.float32) * slots + slot
        chosen.append((place == spot).astype(jnp.float32).astype(jnp.bfloat16))

    for flips in range(1, n_ep):
        back_arrival(flips).wait_recv()

    def mix(i, carry):
        where = pl.ds(pl.multiple_of(i * COLUMN_TILE, COLUMN_TILE), COLUMN_TILE)
        table = back[:, :, where].reshape(n_ep * slots, COLUMN_TILE)
        total = None
        for k in range(2):
            part = jnp.dot(chosen[k], table, preferred_element_type=jnp.float32)
            part = part * route_ref[:, k : k + 1]
            total = part if total is None else total + part
        out_ref[:, where] = total.astype(jnp.bfloat16)
        return carry

    lax.fori_loop(0, outs // COLUMN_TILE, mix, 0)

    for k in range(1, pairs):
        for c in range(2):
            z_copy(k, c).wait_send()
            back_copy(k, c).wait_send()
    pair_copy.wait_send()
    partner_back.wait_send()
    for k in range(pairs):
        for b in range(2):
            if b == 0 and k == 0:
                continue
            for d in range(2):
                for half in range(2):
                    block_copy(b, k, d, half).wait_send()
                relay_copy(b, k, d).wait_send()


def fused_path(
    n_ep, n_tp, tokens, expert_ids, route_weight, norm_gain, gate_weight, up_weight, down_weight
):
    tok_rows, width = tokens.shape
    slots = slots_of(n_ep, tokens.shape, expert_ids.shape)
    hid = gate_weight.shape[2]
    outs = down_weight.shape[2]
    cols = width // n_tp
    pairs = n_ep // 2
    vmem = pl.BlockSpec(memory_space=pltpu.VMEM)
    hbm = pl.BlockSpec(memory_space=pl.ANY)
    dma = pltpu.SemaphoreType.DMA
    return pl.pallas_call(
        functools.partial(fused_kernel, n_ep, n_tp, slots),
        out_shape=jax.ShapeDtypeStruct((tok_rows, outs), jnp.bfloat16),
        in_specs=[vmem] * 5 + [hbm] * 3,
        out_specs=vmem,
        scratch_shapes=[
            pltpu.VMEM(gate_weight.shape[1:], jnp.bfloat16),
            pltpu.VMEM(up_weight.shape[1:], jnp.bfloat16),
            pltpu.VMEM(down_weight.shape[1:], jnp.bfloat16),
            pltpu.VMEM((tok_rows, width), jnp.bfloat16),
            pltpu.VMEM((pairs - 1, 2, slots, cols), jnp.bfloat16),
            pltpu.VMEM((n_tp, slots, cols), jnp.bfloat16),
            pltpu.VMEM((pairs, n_tp, 2, slots, cols), jnp.bfloat16),
            pltpu.VMEM((pairs, n_tp, 2, slots, hid), jnp.bfloat16),
            pltpu.VMEM((pairs, 2, slots, outs), jnp.bfloat16),
            pltpu.VMEM((n_ep, slots, outs), jnp.bfloat16),
            dma((3,)),
            dma((pairs, 2)),
            dma((pairs, 2)),
            dma,
            dma,
            dma((2, pairs, 6)),
            dma((2, pairs, 6)),
            dma((pairs, 2)),
            dma((n_ep,)),
        ],
        compiler_params=pltpu.CompilerParams(
            collective_id=0, has_side_effects=True, vmem_limit_bytes=VMEM_BYTES
        ),
    )(
        tokens,
        expert_ids,
        jnp.transpose(expert_ids),
        route_weight,
        norm_gain.reshape(1, width),
        gate_weight,
        up_weight,
        down_weight,
    )


def slots_of(n_ep, token_shape, id_shape):
    capacity = 5 * token_shape[0] * id_shape[1] // (4 * n_ep)
    return -(-capacity // 16) * 16


def on_device(tokens, expert_ids, route_weight, norm_gain, gate_weight, up_weight, down_weight):
    n_ep = lax.axis_size("ep")
    n_tp = lax.axis_size("tp")
    args = (tokens, expert_ids, route_weight, norm_gain, gate_weight, up_weight, down_weight)
    fits = n_tp == 4 and n_ep >= 4 and n_ep & (n_ep - 1) == 0 and gate_weight.shape[0] == 1
    if fits and expert_ids.shape[1] == 2:
        return fused_path(n_ep, n_tp, *args)
    return plain_path(*args)


def solution(mesh):
    placed = (
        P("ep", None),
        P("ep", None),
        P("ep", None),
        P(),
        P("ep", None, "tp"),
        P("ep", None, "tp"),
        P("ep", None, "tp"),
    )
    return jax.shard_map(
        on_device, mesh=mesh, in_specs=placed, out_specs=P("ep", "tp"), check_vma=False
    )
```

```python
import functools

import jax
import jax.numpy as jnp
from jax import lax
from jax.experimental import pallas as pl
from jax.experimental.pallas import tpu as pltpu
from jax.sharding import PartitionSpec as P

EPS = 1e-06
LIMIT = 7.0
ALPHA = 1.702


def rms_norm(tokens, norm_gain):
    values = tokens.astype(jnp.float32)
    scale = lax.rsqrt(jnp.mean(values * values, axis=-1, keepdims=True) + EPS)
    return (values * scale * norm_gain).astype(jnp.bfloat16)


def clamped_unit(gate_pre, up_pre):
    gate = jnp.minimum(gate_pre, LIMIT)
    up_part = jnp.clip(up_pre, -LIMIT, LIMIT)
    return ((up_part + 1.0) * gate * jax.nn.sigmoid(ALPHA * gate)).astype(jnp.bfloat16)


def slot_numbers(id_blocks, experts, capacity):
    onehot = (id_blocks[:, :, None] == jnp.arange(experts, dtype=jnp.int32)[None, None, :]).astype(
        jnp.int32
    )
    before = jnp.cumsum(onehot, axis=1) - onehot
    position = jnp.sum(before * onehot, axis=2)
    return id_blocks * capacity + position


def project_down(hidden, down_weight):
    result = jnp.einsum(
        "sejf,efd->sejd",
        lax.all_gather(hidden, "tp", axis=3, tiled=True),
        down_weight,
        preferred_element_type=jnp.float32,
    )
    return result.astype(jnp.bfloat16)


def plain_path(tokens, expert_ids, route_weight, norm_gain, gate_weight, up_weight, down_weight):
    n_ep = lax.axis_size("ep")
    n_tp = lax.axis_size("tp")
    tok_rows, width = tokens.shape
    top = expert_ids.shape[1]
    local_experts = gate_weight.shape[0]
    experts = local_experts * n_ep
    capacity = 5 * tok_rows * top // (4 * experts)
    cols = width // n_tp
    normed = rms_norm(tokens, norm_gain)
    dest = slot_numbers(expert_ids.reshape(1, tok_rows * top), experts, capacity).reshape(-1)
    slot_range = jnp.arange(experts * capacity, dtype=jnp.int32)
    match = slot_range[:, None] == dest[None, :]
    pick = jnp.any(match.reshape(experts * capacity, tok_rows, top), axis=2).astype(jnp.bfloat16)
    own = lax.dynamic_slice_in_dim(normed, lax.axis_index("tp") * cols, cols, 1)
    buffer = jnp.dot(pick, own, preferred_element_type=jnp.float32).astype(jnp.bfloat16)
    buffer = buffer.reshape(n_ep, local_experts, capacity, cols)
    arrived = lax.all_to_all(buffer, "ep", split_axis=0, concat_axis=0, tiled=True)
    piece = lax.all_gather(arrived, "tp", axis=3, tiled=True)
    gate_part = jnp.einsum("sejd,edf->sejf", piece, gate_weight, preferred_element_type=jnp.float32)
    up_part = jnp.einsum("sejd,edf->sejf", piece, up_weight, preferred_element_type=jnp.float32)
    hidden = clamped_unit(gate_part, up_part)
    result = project_down(hidden, down_weight)
    back = lax.all_to_all(result, "ep", split_axis=0, concat_axis=0, tiled=True).reshape(
        experts * capacity, cols
    )
    chosen = jnp.transpose(match).astype(jnp.bfloat16)
    per_copy = jnp.dot(chosen, back, preferred_element_type=jnp.float32).reshape(
        tok_rows, top, cols
    )
    mixed = jnp.sum(per_copy * route_weight[:, :, None], axis=1)
    return mixed.astype(jnp.bfloat16)


VMEM_BYTES = 46 * 1024 * 1024
COLUMN_TILE = 256


def flip(value, bits):
    bit = 1
    while bit <= bits:
        if bits & bit:
            value = value + bit - 2 * bit * lax.rem(lax.div(value, jnp.int32(bit)), jnp.int32(2))
        bit *= 2
    return value


def fused_kernel(
    n_ep,
    n_tp,
    slots,
    tokens_hbm,
    ids_row_hbm,
    route_row_hbm,
    gain_hbm,
    gate_hbm,
    up_hbm,
    down_hbm,
    out_ref,
    tokens_ref,
    ids_row_ref,
    route_row_ref,
    gain_ref,
    gate_v,
    up_v,
    down_v,
    scales,
    normed,
    outbox,
    fullbox,
    xbuf,
    hbuf,
    obuf,
    back,
    small_sem,
    weight_sem,
    z_send,
    z_recv,
    pair_send,
    pair_recv,
    g_send,
    g_recv,
    b_send,
    b_recv,
):
    pairs = n_ep // 2
    tok_rows = tokens_ref.shape[0]
    cols = xbuf.shape[-1]
    hid = hbuf.shape[-1]
    outs = obuf.shape[-1]
    ep = lax.axis_index("ep")
    tp = lax.axis_index("tp")
    pair = lax.div(ep, jnp.int32(2))
    core = lax.rem(ep, jnp.int32(2))
    side = (flip(tp, 1), flip(tp, 2))
    far = flip(tp, 3)

    small = (
        (tokens_hbm, tokens_ref),
        (ids_row_hbm, ids_row_ref),
        (route_row_hbm, route_row_ref),
        (gain_hbm, gain_ref),
    )
    small_loads = [
        pltpu.make_async_copy(a, b, small_sem.at[i]) for i, (a, b) in enumerate(small)
    ]
    for load in small_loads:
        load.start()
    loads = [
        pltpu.make_async_copy(hbm.at[0], vmem, weight_sem.at[i])
        for i, (hbm, vmem) in enumerate(((gate_hbm, gate_v), (up_hbm, up_v), (down_hbm, down_v)))
    ]
    for load in loads:
        load.start()

    barrier = pltpu.get_barrier_semaphore()
    for k in range(1, n_ep):
        pl.semaphore_signal(
            barrier, inc=1, device_id=(flip(ep, k), tp), device_id_type=pl.DeviceIdType.MESH
        )
    for other in side:
        pl.semaphore_signal(
            barrier, inc=1, device_id=(ep, other), device_id_type=pl.DeviceIdType.MESH
        )

    for load in small_loads:
        load.wait()

    own_cols = pl.ds(pl.multiple_of(tp * cols, cols), cols)

    def scale_rows(i, carry):
        rows = pl.ds(pl.multiple_of(i * 16, 16), 16)
        values = tokens_ref[rows, :].astype(jnp.float32)
        scale = lax.rsqrt(jnp.mean(values * values, axis=-1, keepdims=True) + EPS)
        scales[rows, :] = jnp.broadcast_to(scale, (16, scales.shape[1]))
        values = tokens_ref[rows, own_cols].astype(jnp.float32)
        normed[rows, own_cols] = (values * scale * gain_ref[:, own_cols]).astype(jnp.bfloat16)
        return carry

    lax.fori_loop(0, tok_rows // 16, scale_rows, 0)

    ids_row = ids_row_ref[...]
    expert_col = lax.broadcasted_iota(jnp.int32, (n_ep, tok_rows), 0)
    hits_row = ((ids_row[0:1, :] == expert_col) | (ids_row[1:2, :] == expert_col)).astype(
        jnp.float32
    ).astype(jnp.bfloat16)
    first = lax.broadcasted_iota(jnp.int32, (tok_rows, tok_rows), 0)
    second = lax.broadcasted_iota(jnp.int32, (tok_rows, tok_rows), 1)
    earlier = (first < second).astype(jnp.float32).astype(jnp.bfloat16)
    before_row = jnp.dot(hits_row, earlier, preferred_element_type=jnp.float32)
    slot_row = [
        jnp.sum(jnp.where(ids_row[k : k + 1, :] == expert_col, before_row, 0.0), axis=0, keepdims=True)
        for k in range(2)
    ]
    slot_at = lax.broadcasted_iota(jnp.int32, (slots, tok_rows), 0).astype(jnp.float32)

    def pick_of(expert):
        taken = ((ids_row[0:1, :] == expert) & (slot_row[0] == slot_at)) | (
            (ids_row[1:2, :] == expert) & (slot_row[1] == slot_at)
        )
        return taken.astype(jnp.float32).astype(jnp.bfloat16)

    pl.semaphore_wait(barrier, n_ep - 1 + 2)

    def z_copy(k, c):
        return pltpu.make_async_remote_copy(
            src_ref=outbox.at[k - 1, c],
            dst_ref=xbuf.at[k, tp, core],
            send_sem=z_send.at[k, c],
            recv_sem=z_recv.at[k, core],
            device_id=(flip(pair, k) * 2 + c, tp),
            device_id_type=pl.DeviceIdType.MESH,
        )

    def z_arrival(k, c):
        return pltpu.make_async_remote_copy(
            src_ref=outbox.at[k - 1, c],
            dst_ref=xbuf.at[k, tp, c],
            send_sem=z_send.at[k, c],
            recv_sem=z_recv.at[k, c],
            device_id=(flip(pair, k) * 2 + c, tp),
            device_id_type=pl.DeviceIdType.MESH,
        )

    for k in range(1, pairs):
        for c in range(2):
            outbox[k - 1, c] = jnp.dot(
                pick_of(flip(pair, k) * 2 + c),
                normed[:, own_cols],
                preferred_element_type=jnp.float32,
            ).astype(jnp.bfloat16)
            z_copy(k, c).start()

    def norm_rows(i, carry):
        rows = pl.ds(pl.multiple_of(i * 16, 16), 16)
        values = tokens_ref[rows, :].astype(jnp.float32)
        normed[rows, :] = (values * scales[rows, 0:1] * gain_ref[...]).astype(jnp.bfloat16)
        return carry

    lax.fori_loop(0, tok_rows // 16, norm_rows, 0)

    partner = flip(ep, 1)
    pair_copy = pltpu.make_async_remote_copy(
        src_ref=fullbox,
        dst_ref=xbuf.at[0, :, core],
        send_sem=pair_send,
        recv_sem=pair_recv,
        device_id=(partner, tp),
        device_id_type=pl.DeviceIdType.MESH,
    )
    pair_arrival = pltpu.make_async_remote_copy(
        src_ref=fullbox,
        dst_ref=xbuf.at[0, :, 1 - core],
        send_sem=pair_send,
        recv_sem=pair_recv,
        device_id=(partner, tp),
        device_id_type=pl.DeviceIdType.MESH,
    )
    theirs = pick_of(partner)
    for j in range(n_tp):
        fullbox[j] = jnp.dot(
            theirs, normed[:, j * cols : (j + 1) * cols], preferred_element_type=jnp.float32
        ).astype(jnp.bfloat16)
    pair_copy.start()
    mine = pick_of(ep)
    for j in range(n_tp):
        xbuf[0, j, core] = jnp.dot(
            mine, normed[:, j * cols : (j + 1) * cols], preferred_element_type=jnp.float32
        ).astype(jnp.bfloat16)

    boxes = (xbuf, hbuf)

    def block_copy(b, k, d, half):
        return pltpu.make_async_remote_copy(
            src_ref=boxes[b].at[k, tp, half],
            dst_ref=boxes[b].at[k, tp, half],
            send_sem=g_send.at[b, k, 2 * d + half],
            recv_sem=g_recv.at[b, k, 2 * d + half],
            device_id=(ep, side[d]),
            device_id_type=pl.DeviceIdType.MESH,
        )

    def block_arrival(b, k, d, half):
        return pltpu.make_async_remote_copy(
            src_ref=boxes[b].at[k, side[d], half],
            dst_ref=boxes[b].at[k, side[d], half],
            send_sem=g_send.at[b, k, 2 * d + half],
            recv_sem=g_recv.at[b, k, 2 * d + half],
            device_id=(ep, side[d]),
            device_id_type=pl.DeviceIdType.MESH,
        )

    def relay_copy(b, k, d):
        return pltpu.make_async_remote_copy(
            src_ref=boxes[b].at[k, side[d], d],
            dst_ref=boxes[b].at[k, side[d], d],
            send_sem=g_send.at[b, k, 4 + d],
            recv_sem=g_recv.at[b, k, 4 + d],
            device_id=(ep, side[1 - d]),
            device_id_type=pl.DeviceIdType.MESH,
        )

    def relay_arrival(b, k, d):
        return pltpu.make_async_remote_copy(
            src_ref=boxes[b].at[k, far, d],
            dst_ref=boxes[b].at[k, far, d],
            send_sem=g_send.at[b, k, 4 + d],
            recv_sem=g_recv.at[b, k, 4 + d],
            device_id=(ep, side[1 - d]),
            device_id_type=pl.DeviceIdType.MESH,
        )

    def spread(b, k):
        for step in range(2):
            for d in range(2):
                block_copy(b, k, d, d if step == 0 else 1 - d).start()

    def relay(b, k):
        for d in range(2):
            block_arrival(b, k, d, d).wait_recv()
            relay_copy(b, k, d).start()

    def gathered(b, k):
        for d in range(2):
            block_arrival(b, k, d, 1 - d).wait_recv()
        for d in range(2):
            relay_arrival(b, k, d).wait_recv()

    def enter(k):
        for c in range(2):
            z_arrival(k, c).wait_recv()
        spread(0, k)

    def dot_blocks(box, k, weight, where):
        depth = box.shape[-1]
        total = None
        for j in range(n_tp):
            part = jnp.dot(
                box[k, j].reshape(2 * slots, depth),
                weight[j * depth : (j + 1) * depth, where],
                preferred_element_type=jnp.float32,
            )
            total = part if total is None else total + part
        return total

    def units(k):
        def tile(i, carry):
            where = pl.ds(pl.multiple_of(i * COLUMN_TILE, COLUMN_TILE), COLUMN_TILE)
            gate_pre = dot_blocks(xbuf, k, gate_v, where)
            up_pre = dot_blocks(xbuf, k, up_v, where)
            hidden = clamped_unit(gate_pre, up_pre)
            hbuf[k, tp, :, :, where] = hidden.reshape(2, slots, COLUMN_TILE)
            return carry

        lax.fori_loop(0, hid // COLUMN_TILE, tile, 0)

    def back_copy(k, c):
        return pltpu.make_async_remote_copy(
            src_ref=obuf.at[k, c],
            dst_ref=back.at[ep],
            send_sem=b_send.at[k, c],
            recv_sem=b_recv.at[ep],
            device_id=(flip(pair, k) * 2 + c, tp),
            device_id_type=pl.DeviceIdType.MESH,
        )

    def back_arrival(flips):
        other = flip(ep, flips)
        return pltpu.make_async_remote_copy(
            src_ref=obuf.at[0, 0],
            dst_ref=back.at[other],
            send_sem=b_send.at[0, 0],
            recv_sem=b_recv.at[other],
            device_id=(other, tp),
            device_id_type=pl.DeviceIdType.MESH,
        )

    partner_back = pltpu.make_async_remote_copy(
        src_ref=obuf.at[0, 1 - core],
        dst_ref=back.at[ep],
        send_sem=b_send.at[0, 0],
        recv_sem=b_recv.at[ep],
        device_id=(partner, tp),
        device_id_type=pl.DeviceIdType.MESH,
    )

    def results(k):
        def tile(i, carry):
            where = pl.ds(pl.multiple_of(i * COLUMN_TILE, COLUMN_TILE), COLUMN_TILE)
            total = dot_blocks(hbuf, k, down_v, where).astype(jnp.bfloat16)
            obuf[k, :, :, where] = total.reshape(2, slots, COLUMN_TILE)
            return carry

        lax.fori_loop(0, outs // COLUMN_TILE, tile, 0)
        if k == 0:
            partner_back.start()
            back[ep] = obuf[0, core]
        else:
            for c in range(2):
                back_copy(k, c).start()

    loads[0].wait()
    loads[1].wait()
    pair_arrival.wait_recv()
    units(0)
    enter(1)
    relay(0, 1)
    if pairs > 2:
        enter(2)
    loads[2].wait()
    for k in range(1, pairs):
        gathered(0, k)
        units(k)
        spread(1, k)
        if k + 1 < pairs:
            relay(0, k + 1)
        if k + 2 < pairs:
            enter(k + 2)
        if k == pairs - 1:
            spread(1, 0)
        if k >= 2:
            gathered(1, k - 1)
            results(k - 1)
        relay(1, k)
    gathered(1, pairs - 1)
    results(pairs - 1)
    relay(1, 0)
    gathered(1, 0)
    results(0)

    place = lax.broadcasted_iota(jnp.int32, (n_ep * slots, tok_rows), 0).astype(jnp.float32)
    share = None
    for k in range(2):
        spot = ids_row[k : k + 1, :].astype(jnp.float32) * slots + slot_row[k]
        part = jnp.where(place == spot, route_row_ref[k : k + 1, :], 0.0)
        share = part if share is None else share + part
    share = jnp.transpose(share)
    share_high = share.astype(jnp.bfloat16)
    share_low = (share - share_high.astype(jnp.float32)).astype(jnp.bfloat16)

    for flips in range(1, n_ep):
        back_arrival(flips).wait_recv()

    def mix(i, carry):
        where = pl.ds(pl.multiple_of(i * COLUMN_TILE, COLUMN_TILE), COLUMN_TILE)
        table = back[:, :, where].reshape(n_ep * slots, COLUMN_TILE)
        total = jnp.dot(share_high, table, preferred_element_type=jnp.float32)
        total = total + jnp.dot(share_low, table, preferred_element_type=jnp.float32)
        out_ref[:, where] = total.astype(jnp.bfloat16)
        return carry

    lax.fori_loop(0, outs // COLUMN_TILE, mix, 0)

    for k in range(1, pairs):
        for c in range(2):
            z_copy(k, c).wait_send()
            back_copy(k, c).wait_send()
    pair_copy.wait_send()
    partner_back.wait_send()
    for k in range(pairs):
        for b in range(2):
            if b == 0 and k == 0:
                continue
            for d in range(2):
                for half in range(2):
                    block_copy(b, k, d, half).wait_send()
                relay_copy(b, k, d).wait_send()


def fused_path(
    n_ep, n_tp, tokens, expert_ids, route_weight, norm_gain, gate_weight, up_weight, down_weight
):
    tok_rows, width = tokens.shape
    slots = slots_of(n_ep, tokens.shape, expert_ids.shape)
    hid = gate_weight.shape[2]
    outs = down_weight.shape[2]
    cols = width // n_tp
    pairs = n_ep // 2
    vmem = pl.BlockSpec(memory_space=pltpu.VMEM)
    hbm = pl.BlockSpec(memory_space=pltpu.HBM)
    dma = pltpu.SemaphoreType.DMA
    arrays = (
        tokens,
        jnp.transpose(expert_ids),
        jnp.transpose(route_weight),
        norm_gain.reshape(1, width),
        gate_weight,
        up_weight,
        down_weight,
    )
    return pl.pallas_call(
        functools.partial(fused_kernel, n_ep, n_tp, slots),
        out_shape=jax.ShapeDtypeStruct((tok_rows, outs), jnp.bfloat16),
        in_specs=[hbm] * 7,
        out_specs=vmem,
        scratch_shapes=[
            pltpu.VMEM(tokens.shape, tokens.dtype),
            pltpu.VMEM(expert_ids.shape[::-1], expert_ids.dtype),
            pltpu.VMEM(route_weight.shape[::-1], route_weight.dtype),
            pltpu.VMEM((1, width), norm_gain.dtype),
            pltpu.VMEM(gate_weight.shape[1:], jnp.bfloat16),
            pltpu.VMEM(up_weight.shape[1:], jnp.bfloat16),
            pltpu.VMEM(down_weight.shape[1:], jnp.bfloat16),
            pltpu.VMEM((tok_rows, 128), jnp.float32),
            pltpu.VMEM((tok_rows, width), jnp.bfloat16),
            pltpu.VMEM((pairs - 1, 2, slots, cols), jnp.bfloat16),
            pltpu.VMEM((n_tp, slots, cols), jnp.bfloat16),
            pltpu.VMEM((pairs, n_tp, 2, slots, cols), jnp.bfloat16),
            pltpu.VMEM((pairs, n_tp, 2, slots, hid), jnp.bfloat16),
            pltpu.VMEM((pairs, 2, slots, outs), jnp.bfloat16),
            pltpu.VMEM((n_ep, slots, outs), jnp.bfloat16),
            dma((4,)),
            dma((3,)),
            dma((pairs, 2)),
            dma((pairs, 2)),
            dma,
            dma,
            dma((2, pairs, 6)),
            dma((2, pairs, 6)),
            dma((pairs, 2)),
            dma((n_ep,)),
        ],
        compiler_params=pltpu.CompilerParams(
            collective_id=0, has_side_effects=True, vmem_limit_bytes=VMEM_BYTES
        ),
    )(*(pltpu.with_memory_space_constraint(array, pltpu.HBM) for array in arrays))


def slots_of(n_ep, token_shape, id_shape):
    capacity = 5 * token_shape[0] * id_shape[1] // (4 * n_ep)
    return -(-capacity // 16) * 16


def on_device(tokens, expert_ids, route_weight, norm_gain, gate_weight, up_weight, down_weight):
    n_ep = lax.axis_size("ep")
    n_tp = lax.axis_size("tp")
    args = (tokens, expert_ids, route_weight, norm_gain, gate_weight, up_weight, down_weight)
    fits = n_tp == 4 and n_ep >= 4 and n_ep & (n_ep - 1) == 0 and gate_weight.shape[0] == 1
    if fits and expert_ids.shape[1] == 2:
        return fused_path(n_ep, n_tp, *args)
    return plain_path(*args)


def solution(mesh):
    placed = (
        P("ep", None),
        P("ep", None),
        P("ep", None),
        P(),
        P("ep", None, "tp"),
        P("ep", None, "tp"),
        P("ep", None, "tp"),
    )
    return jax.shard_map(
        on_device, mesh=mesh, in_specs=placed, out_specs=P("ep", "tp"), check_vma=False
    )
```

```python
import functools

import jax
import jax.numpy as jnp
from jax import lax
from jax.experimental import pallas as pl
from jax.experimental.pallas import tpu as pltpu
from jax.sharding import PartitionSpec as P

EPS = 1e-06
LIMIT = 7.0
ALPHA = 1.702


def rms_norm(tokens, norm_gain):
    values = tokens.astype(jnp.float32)
    scale = lax.rsqrt(jnp.mean(values * values, axis=-1, keepdims=True) + EPS)
    return (values * scale * norm_gain).astype(jnp.bfloat16)


def clamped_unit(gate_pre, up_pre):
    gate = jnp.minimum(gate_pre, LIMIT)
    up_part = jnp.clip(up_pre, -LIMIT, LIMIT)
    return ((up_part + 1.0) * gate * jax.nn.sigmoid(ALPHA * gate)).astype(jnp.bfloat16)


def slot_numbers(id_blocks, experts, capacity):
    onehot = (id_blocks[:, :, None] == jnp.arange(experts, dtype=jnp.int32)[None, None, :]).astype(
        jnp.int32
    )
    before = jnp.cumsum(onehot, axis=1) - onehot
    position = jnp.sum(before * onehot, axis=2)
    return id_blocks * capacity + position


def project_down(hidden, down_weight):
    result = jnp.einsum(
        "sejf,efd->sejd",
        lax.all_gather(hidden, "tp", axis=3, tiled=True),
        down_weight,
        preferred_element_type=jnp.float32,
    )
    return result.astype(jnp.bfloat16)


def plain_path(tokens, expert_ids, route_weight, norm_gain, gate_weight, up_weight, down_weight):
    n_ep = lax.axis_size("ep")
    n_tp = lax.axis_size("tp")
    tok_rows, width = tokens.shape
    top = expert_ids.shape[1]
    local_experts = gate_weight.shape[0]
    experts = local_experts * n_ep
    capacity = 5 * tok_rows * top // (4 * experts)
    cols = width // n_tp
    normed = rms_norm(tokens, norm_gain)
    dest = slot_numbers(expert_ids.reshape(1, tok_rows * top), experts, capacity).reshape(-1)
    slot_range = jnp.arange(experts * capacity, dtype=jnp.int32)
    match = slot_range[:, None] == dest[None, :]
    pick = jnp.any(match.reshape(experts * capacity, tok_rows, top), axis=2).astype(jnp.bfloat16)
    own = lax.dynamic_slice_in_dim(normed, lax.axis_index("tp") * cols, cols, 1)
    buffer = jnp.dot(pick, own, preferred_element_type=jnp.float32).astype(jnp.bfloat16)
    buffer = buffer.reshape(n_ep, local_experts, capacity, cols)
    arrived = lax.all_to_all(buffer, "ep", split_axis=0, concat_axis=0, tiled=True)
    piece = lax.all_gather(arrived, "tp", axis=3, tiled=True)
    gate_part = jnp.einsum("sejd,edf->sejf", piece, gate_weight, preferred_element_type=jnp.float32)
    up_part = jnp.einsum("sejd,edf->sejf", piece, up_weight, preferred_element_type=jnp.float32)
    hidden = clamped_unit(gate_part, up_part)
    result = project_down(hidden, down_weight)
    back = lax.all_to_all(result, "ep", split_axis=0, concat_axis=0, tiled=True).reshape(
        experts * capacity, cols
    )
    chosen = jnp.transpose(match).astype(jnp.bfloat16)
    per_copy = jnp.dot(chosen, back, preferred_element_type=jnp.float32).reshape(
        tok_rows, top, cols
    )
    mixed = jnp.sum(per_copy * route_weight[:, :, None], axis=1)
    return mixed.astype(jnp.bfloat16)


VMEM_BYTES = 48 * 1024 * 1024
COLUMN_TILE = 256


def flip(value, bits):
    bit = 1
    while bit <= bits:
        if bits & bit:
            value = value + bit - 2 * bit * lax.rem(lax.div(value, jnp.int32(bit)), jnp.int32(2))
        bit *= 2
    return value


def fused_kernel(
    n_ep,
    n_tp,
    slots,
    tokens_hbm,
    ids_row_hbm,
    route_row_hbm,
    gain_hbm,
    gate_hbm,
    up_hbm,
    down_hbm,
    out_ref,
    tokens_ref,
    ids_row_ref,
    route_row_ref,
    gain_ref,
    gate_v,
    up_v,
    down_v,
    scales,
    normed,
    outbox,
    fullbox,
    xbuf,
    hbuf,
    obuf,
    back,
    small_sem,
    weight_sem,
    z_send,
    z_recv,
    pair_send,
    pair_recv,
    g_send,
    g_recv,
    b_send,
    b_recv,
):
    pairs = n_ep // 2
    tok_rows = tokens_ref.shape[0]
    cols = xbuf.shape[-1]
    hid = hbuf.shape[-1]
    outs = obuf.shape[-1]
    ep = lax.axis_index("ep")
    tp = lax.axis_index("tp")
    pair = lax.div(ep, jnp.int32(2))
    core = lax.rem(ep, jnp.int32(2))
    side = (flip(tp, 1), flip(tp, 2))
    far = flip(tp, 3)

    small = (
        (tokens_hbm, tokens_ref),
        (ids_row_hbm, ids_row_ref),
        (route_row_hbm, route_row_ref),
        (gain_hbm, gain_ref),
    )
    small_loads = [
        pltpu.make_async_copy(a, b, small_sem.at[i]) for i, (a, b) in enumerate(small)
    ]
    for load in small_loads:
        load.start()
    loads = [
        pltpu.make_async_copy(hbm.at[0], vmem, weight_sem.at[i])
        for i, (hbm, vmem) in enumerate(((gate_hbm, gate_v), (up_hbm, up_v), (down_hbm, down_v)))
    ]
    for load in loads:
        load.start()

    barrier = pltpu.get_barrier_semaphore()
    for k in range(1, n_ep):
        pl.semaphore_signal(
            barrier, inc=1, device_id=(flip(ep, k), tp), device_id_type=pl.DeviceIdType.MESH
        )
    for other in side:
        pl.semaphore_signal(
            barrier, inc=1, device_id=(ep, other), device_id_type=pl.DeviceIdType.MESH
        )

    for load in small_loads:
        load.wait()

    own_cols = pl.ds(pl.multiple_of(tp * cols, cols), cols)

    def scale_rows(i, carry):
        rows = pl.ds(pl.multiple_of(i * 32, 32), 32)
        values = tokens_ref[rows, :].astype(jnp.float32)
        scale = lax.rsqrt(jnp.mean(values * values, axis=-1, keepdims=True) + EPS)
        scales[rows, :] = jnp.broadcast_to(scale, (32, scales.shape[1]))
        values = tokens_ref[rows, own_cols].astype(jnp.float32)
        normed[rows, own_cols] = (values * scale * gain_ref[:, own_cols]).astype(jnp.bfloat16)
        return carry

    lax.fori_loop(0, tok_rows // 32, scale_rows, 0)

    ids_row = ids_row_ref[...]
    expert_col = lax.broadcasted_iota(jnp.int32, (n_ep, tok_rows), 0)
    hits_row = ((ids_row[0:1, :] == expert_col) | (ids_row[1:2, :] == expert_col)).astype(
        jnp.float32
    ).astype(jnp.bfloat16)
    first = lax.broadcasted_iota(jnp.int32, (tok_rows, tok_rows), 0)
    second = lax.broadcasted_iota(jnp.int32, (tok_rows, tok_rows), 1)
    earlier = (first < second).astype(jnp.float32).astype(jnp.bfloat16)
    before_row = jnp.dot(hits_row, earlier, preferred_element_type=jnp.float32)
    slot_row = [
        jnp.sum(jnp.where(ids_row[k : k + 1, :] == expert_col, before_row, 0.0), axis=0, keepdims=True)
        for k in range(2)
    ]
    slot_at = lax.broadcasted_iota(jnp.int32, (slots, tok_rows), 0).astype(jnp.float32)

    def pick_of(expert):
        taken = ((ids_row[0:1, :] == expert) & (slot_row[0] == slot_at)) | (
            (ids_row[1:2, :] == expert) & (slot_row[1] == slot_at)
        )
        return taken.astype(jnp.float32).astype(jnp.bfloat16)

    pl.semaphore_wait(barrier, n_ep - 1 + 2)

    def z_copy(k, c):
        return pltpu.make_async_remote_copy(
            src_ref=outbox.at[k - 2, c],
            dst_ref=xbuf.at[k, tp, core],
            send_sem=z_send.at[k, c],
            recv_sem=z_recv.at[k, core],
            device_id=(flip(pair, k) * 2 + c, tp),
            device_id_type=pl.DeviceIdType.MESH,
        )

    def z_arrival(k, c):
        return pltpu.make_async_remote_copy(
            src_ref=outbox.at[k - 2, c],
            dst_ref=xbuf.at[k, tp, c],
            send_sem=z_send.at[k, c],
            recv_sem=z_recv.at[k, c],
            device_id=(flip(pair, k) * 2 + c, tp),
            device_id_type=pl.DeviceIdType.MESH,
        )

    away = [(k, c) for k in range(2, pairs) for c in range(2)]
    if away:
        picks = jnp.concatenate([pick_of(flip(pair, k) * 2 + c) for k, c in away], axis=0)
        rows_out = jnp.dot(
            picks, normed[:, own_cols], preferred_element_type=jnp.float32
        ).astype(jnp.bfloat16)
        for at, (k, c) in enumerate(away):
            outbox[k - 2, c] = rows_out[at * slots : (at + 1) * slots]
        for k, c in away:
            z_copy(k, c).start()

    def norm_rows(i, carry):
        rows = pl.ds(pl.multiple_of(i * 16, 16), 16)
        values = tokens_ref[rows, :].astype(jnp.float32)
        normed[rows, :] = (values * scales[rows, 0:1] * gain_ref[...]).astype(jnp.bfloat16)
        return carry

    lax.fori_loop(0, tok_rows // 16, norm_rows, 0)

    partner = flip(ep, 1)
    pair_copy = pltpu.make_async_remote_copy(
        src_ref=fullbox.at[2],
        dst_ref=xbuf.at[0, :, core],
        send_sem=pair_send,
        recv_sem=pair_recv,
        device_id=(partner, tp),
        device_id_type=pl.DeviceIdType.MESH,
    )
    pair_arrival = pltpu.make_async_remote_copy(
        src_ref=fullbox.at[2],
        dst_ref=xbuf.at[0, :, 1 - core],
        send_sem=pair_send,
        recv_sem=pair_recv,
        device_id=(partner, tp),
        device_id_type=pl.DeviceIdType.MESH,
    )

    def whole_copy(c):
        return pltpu.make_async_remote_copy(
            src_ref=fullbox.at[c],
            dst_ref=xbuf.at[1, :, core],
            send_sem=z_send.at[1, c],
            recv_sem=z_recv.at[1, core],
            device_id=(flip(pair, 1) * 2 + c, tp),
            device_id_type=pl.DeviceIdType.MESH,
        )

    def whole_arrival(c):
        return pltpu.make_async_remote_copy(
            src_ref=fullbox.at[c],
            dst_ref=xbuf.at[1, :, c],
            send_sem=z_send.at[1, c],
            recv_sem=z_recv.at[1, c],
            device_id=(flip(pair, 1) * 2 + c, tp),
            device_id_type=pl.DeviceIdType.MESH,
        )

    near = flip(pair, 1) * 2
    picks = jnp.concatenate(
        [pick_of(near), pick_of(near + 1), pick_of(partner), pick_of(ep)], axis=0
    )
    for j in range(n_tp):
        whole = jnp.dot(
            picks, normed[:, j * cols : (j + 1) * cols], preferred_element_type=jnp.float32
        ).astype(jnp.bfloat16)
        for at in range(3):
            fullbox[at, j] = whole[at * slots : (at + 1) * slots]
        xbuf[0, j, core] = whole[3 * slots :]
    pair_copy.start()
    for c in range(2):
        whole_copy(c).start()

    boxes = (xbuf, hbuf)
    part_a, part_b = (1 - core, 0), (core, pairs)
    piece = slots // 2

    def place_of(b, k, j, half, part):
        if part is None:
            return boxes[b].at[k, j, half]
        return boxes[b].at[k, j, part[0], pl.ds(half * piece, piece)]

    def sems_of(b, k, at, part):
        row = k if part is None else part[1]
        return {"send_sem": g_send.at[b, row, at], "recv_sem": g_recv.at[b, row, at]}

    def block_copy(b, k, d, half, part):
        return pltpu.make_async_remote_copy(
            src_ref=place_of(b, k, tp, half, part),
            dst_ref=place_of(b, k, tp, half, part),
            device_id=(ep, side[d]),
            device_id_type=pl.DeviceIdType.MESH,
            **sems_of(b, k, 2 * d + half, part),
        )

    def block_arrival(b, k, d, half, part):
        return pltpu.make_async_remote_copy(
            src_ref=place_of(b, k, side[d], half, part),
            dst_ref=place_of(b, k, side[d], half, part),
            device_id=(ep, side[d]),
            device_id_type=pl.DeviceIdType.MESH,
            **sems_of(b, k, 2 * d + half, part),
        )

    def relay_copy(b, k, d, part):
        return pltpu.make_async_remote_copy(
            src_ref=place_of(b, k, side[d], d, part),
            dst_ref=place_of(b, k, side[d], d, part),
            device_id=(ep, side[1 - d]),
            device_id_type=pl.DeviceIdType.MESH,
            **sems_of(b, k, 4 + d, part),
        )

    def relay_arrival(b, k, d, part):
        return pltpu.make_async_remote_copy(
            src_ref=place_of(b, k, far, d, part),
            dst_ref=place_of(b, k, far, d, part),
            device_id=(ep, side[1 - d]),
            device_id_type=pl.DeviceIdType.MESH,
            **sems_of(b, k, 4 + d, part),
        )

    def spread(b, k, part=None):
        for step in range(2):
            for d in range(2):
                block_copy(b, k, d, d if step == 0 else 1 - d, part).start()

    def relay(b, k, part=None):
        for d in range(2):
            block_arrival(b, k, d, d, part).wait_recv()
            relay_copy(b, k, d, part).start()

    def gathered(b, k, part=None):
        for d in range(2):
            block_arrival(b, k, d, 1 - d, part).wait_recv()
        for d in range(2):
            relay_arrival(b, k, d, part).wait_recv()

    def enter(k):
        for c in range(2):
            z_arrival(k, c).wait_recv()
        spread(0, k)

    def dot_blocks(box, k, weight, where, part=None):
        depth = box.shape[-1]
        total = None
        for j in range(n_tp):
            term = jnp.dot(
                box[k, j].reshape(2 * slots, depth) if part is None else box[k, j, part[0]],
                weight[j * depth : (j + 1) * depth, where],
                preferred_element_type=jnp.float32,
            )
            total = term if total is None else total + term
        return total

    def units(k):
        def tile(i, carry):
            where = pl.ds(pl.multiple_of(i * COLUMN_TILE, COLUMN_TILE), COLUMN_TILE)
            gate_pre = dot_blocks(xbuf, k, gate_v, where)
            up_pre = dot_blocks(xbuf, k, up_v, where)
            hidden = clamped_unit(gate_pre, up_pre)
            hbuf[k, tp, :, :, where] = hidden.reshape(2, slots, COLUMN_TILE)
            return carry

        lax.fori_loop(0, hid // COLUMN_TILE, tile, 0)

    def back_copy(k, c):
        return pltpu.make_async_remote_copy(
            src_ref=obuf.at[k, c],
            dst_ref=back.at[ep],
            send_sem=b_send.at[k, c],
            recv_sem=b_recv.at[ep],
            device_id=(flip(pair, k) * 2 + c, tp),
            device_id_type=pl.DeviceIdType.MESH,
        )

    def back_arrival(flips):
        other = flip(ep, flips)
        return pltpu.make_async_remote_copy(
            src_ref=obuf.at[0, 0],
            dst_ref=back.at[other],
            send_sem=b_send.at[0, 0],
            recv_sem=b_recv.at[other],
            device_id=(other, tp),
            device_id_type=pl.DeviceIdType.MESH,
        )

    partner_back = pltpu.make_async_remote_copy(
        src_ref=obuf.at[0, 0],
        dst_ref=back.at[ep],
        send_sem=b_send.at[0, 0],
        recv_sem=b_recv.at[ep],
        device_id=(partner, tp),
        device_id_type=pl.DeviceIdType.MESH,
    )

    def results(k):
        def tile(i, carry):
            where = pl.ds(pl.multiple_of(i * COLUMN_TILE, COLUMN_TILE), COLUMN_TILE)
            total = dot_blocks(hbuf, k, down_v, where).astype(jnp.bfloat16)
            obuf[k, :, :, where] = total.reshape(2, slots, COLUMN_TILE)
            return carry

        lax.fori_loop(0, outs // COLUMN_TILE, tile, 0)
        for c in range(2):
            back_copy(k, c).start()

    def own_results(part, store):
        def tile(i, carry):
            where = pl.ds(pl.multiple_of(i * COLUMN_TILE, COLUMN_TILE), COLUMN_TILE)
            store(where, dot_blocks(hbuf, 0, down_v, where, part).astype(jnp.bfloat16))
            return carry

        lax.fori_loop(0, outs // COLUMN_TILE, tile, 0)

    def store_partner(where, total):
        obuf[0, 0, :, where] = total

    def store_own(where, total):
        back[ep, :, where] = total

    loads[0].wait()
    loads[1].wait()
    pair_arrival.wait_recv()
    units(0)
    spread(1, 0, part_a)
    if pairs > 2:
        enter(2)
    relay(1, 0, part_a)
    loads[2].wait()
    gathered(1, 0, part_a)
    own_results(part_a, store_partner)
    partner_back.start()
    for k in range(2, pairs):
        if k == 2:
            relay(0, k)
        if k + 1 < pairs:
            enter(k + 1)
        gathered(0, k)
        units(k)
        if k + 1 < pairs:
            relay(0, k + 1)
        spread(1, k)
        if k > 2:
            relay(1, k - 1)
            gathered(1, k - 1)
            results(k - 1)
    for c in range(2):
        whole_arrival(c).wait_recv()
    units(1)
    spread(1, 1)
    spread(1, 0, part_b)
    if pairs > 2:
        relay(1, pairs - 1)
        gathered(1, pairs - 1)
        results(pairs - 1)
    relay(1, 1)
    gathered(1, 1)
    results(1)
    relay(1, 0, part_b)
    gathered(1, 0, part_b)
    own_results(part_b, store_own)

    place = lax.broadcasted_iota(jnp.int32, (n_ep * slots, tok_rows), 0).astype(jnp.float32)
    share = None
    for k in range(2):
        spot = ids_row[k : k + 1, :].astype(jnp.float32) * slots + slot_row[k]
        part = jnp.where(place == spot, route_row_ref[k : k + 1, :], 0.0)
        share = part if share is None else share + part
    share = jnp.transpose(share)
    share_high = share.astype(jnp.bfloat16)
    share_low = (share - share_high.astype(jnp.float32)).astype(jnp.bfloat16)

    for flips in range(1, n_ep):
        back_arrival(flips).wait_recv()

    def mix(i, carry):
        where = pl.ds(pl.multiple_of(i * COLUMN_TILE, COLUMN_TILE), COLUMN_TILE)
        table = back[:, :, where].reshape(n_ep * slots, COLUMN_TILE)
        total = jnp.dot(share_high, table, preferred_element_type=jnp.float32)
        total = total + jnp.dot(share_low, table, preferred_element_type=jnp.float32)
        out_ref[:, where] = total.astype(jnp.bfloat16)
        return carry

    lax.fori_loop(0, outs // COLUMN_TILE, mix, 0)

    for k in range(1, pairs):
        for c in range(2):
            if k > 1:
                z_copy(k, c).wait_send()
            else:
                whole_copy(c).wait_send()
            back_copy(k, c).wait_send()
    pair_copy.wait_send()
    partner_back.wait_send()
    sent = [(0, k, None) for k in range(2, pairs)] + [(1, k, None) for k in range(1, pairs)]
    for b, k, part in sent + [(1, 0, part_a), (1, 0, part_b)]:
        for d in range(2):
            for half in range(2):
                block_copy(b, k, d, half, part).wait_send()
            relay_copy(b, k, d, part).wait_send()


def fused_path(
    n_ep, n_tp, tokens, expert_ids, route_weight, norm_gain, gate_weight, up_weight, down_weight
):
    tok_rows, width = tokens.shape
    slots = slots_of(n_ep, tokens.shape, expert_ids.shape)
    hid = gate_weight.shape[2]
    outs = down_weight.shape[2]
    cols = width // n_tp
    pairs = n_ep // 2
    vmem = pl.BlockSpec(memory_space=pltpu.VMEM)
    hbm = pl.BlockSpec(memory_space=pltpu.HBM)
    dma = pltpu.SemaphoreType.DMA
    arrays = (
        tokens,
        jnp.transpose(expert_ids),
        jnp.transpose(route_weight),
        norm_gain.reshape(1, width),
        gate_weight,
        up_weight,
        down_weight,
    )
    return pl.pallas_call(
        functools.partial(fused_kernel, n_ep, n_tp, slots),
        out_shape=jax.ShapeDtypeStruct((tok_rows, outs), jnp.bfloat16),
        in_specs=[hbm] * 7,
        out_specs=vmem,
        scratch_shapes=[
            pltpu.VMEM(tokens.shape, tokens.dtype),
            pltpu.VMEM(expert_ids.shape[::-1], expert_ids.dtype),
            pltpu.VMEM(route_weight.shape[::-1], route_weight.dtype),
            pltpu.VMEM((1, width), norm_gain.dtype),
            pltpu.VMEM(gate_weight.shape[1:], jnp.bfloat16),
            pltpu.VMEM(up_weight.shape[1:], jnp.bfloat16),
            pltpu.VMEM(down_weight.shape[1:], jnp.bfloat16),
            pltpu.VMEM((tok_rows, 128), jnp.float32),
            pltpu.VMEM((tok_rows, width), jnp.bfloat16),
            pltpu.VMEM((max(pairs - 2, 1), 2, slots, cols), jnp.bfloat16),
            pltpu.VMEM((3, n_tp, slots, cols), jnp.bfloat16),
            pltpu.VMEM((pairs, n_tp, 2, slots, cols), jnp.bfloat16),
            pltpu.VMEM((pairs, n_tp, 2, slots, hid), jnp.bfloat16),
            pltpu.VMEM((pairs, 2, slots, outs), jnp.bfloat16),
            pltpu.VMEM((n_ep, slots, outs), jnp.bfloat16),
            dma((4,)),
            dma((3,)),
            dma((pairs, 2)),
            dma((pairs, 2)),
            dma,
            dma,
            dma((2, pairs + 1, 6)),
            dma((2, pairs + 1, 6)),
            dma((pairs, 2)),
            dma((n_ep,)),
        ],
        compiler_params=pltpu.CompilerParams(
            collective_id=0, has_side_effects=True, vmem_limit_bytes=VMEM_BYTES
        ),
    )(*(pltpu.with_memory_space_constraint(array, pltpu.HBM) for array in arrays))


def slots_of(n_ep, token_shape, id_shape):
    capacity = 5 * token_shape[0] * id_shape[1] // (4 * n_ep)
    return -(-capacity // 32) * 32


def on_device(tokens, expert_ids, route_weight, norm_gain, gate_weight, up_weight, down_weight):
    n_ep = lax.axis_size("ep")
    n_tp = lax.axis_size("tp")
    args = (tokens, expert_ids, route_weight, norm_gain, gate_weight, up_weight, down_weight)
    fits = n_tp == 4 and tokens.shape[0] % 32 == 0 and n_ep >= 4 and n_ep & (n_ep - 1) == 0 and gate_weight.shape[0] == 1
    if fits and expert_ids.shape[1] == 2:
        return fused_path(n_ep, n_tp, *args)
    return plain_path(*args)


def solution(mesh):
    placed = (
        P("ep", None),
        P("ep", None),
        P("ep", None),
        P(),
        P("ep", None, "tp"),
        P("ep", None, "tp"),
        P("ep", None, "tp"),
    )
    return jax.shard_map(
        on_device, mesh=mesh, in_specs=placed, out_specs=P("ep", "tp"), check_vma=False
    )
```
